32 devices in a mesh: kv: 8 (over z, y), tp: 4 (over x, core).
Axes of the slice: x: 2, y: 2, z: 4, core: 2. Of those that a mesh axis runs over, the one named last changes fastest.
Arguments:
- tokens: bfloat16 [128, 4096], P('tp', 'kv')
- seq_pos: int32 [128], P('kv'), may hold values from 0 to 4095
- state: float32 [128, 16, 128, 256], P('kv', 'tp'), may hold values from -0.6 to 0.6
- norm_in_gain: float32 [4096], P('kv'), may hold values from 0.1 to 1.9
- query_weight: bfloat16 [4096, 2048], P('kv', 'tp'), may hold values from -0.09375 to 0.09375
- key_weight: bfloat16 [4096, 2048], P('kv', 'tp'), may hold values from -0.09375 to 0.09375
- value_weight: bfloat16 [4096, 4096], P('kv', 'tp'), may hold values from -0.09375 to 0.09375
- gate_weight: bfloat16 [4096, 4096], P('kv', 'tp'), may hold values from -0.09375 to 0.09375
- head_gain: float32 [4096], P('tp'), may hold values from 0.1 to 1.9
- out_weight: bfloat16 [4096, 4096], P('tp', 'kv'), may hold values from -0.09375 to 0.09375
- norm_mlp_gain: float32 [4096], P('kv'), may hold values from 0.1 to 1.9
- hidden_weight: bfloat16 [4096, 16384], P('kv', 'tp'), may hold values from -0.09375 to 0.09375
- down_weight: bfloat16 [16384, 4096], P('tp', 'kv'), may hold values from -0.046875 to 0.046875
Outputs:
- output: bfloat16 [128, 4096], P('tp', 'kv')
- new_state: float32 [128, 16, 128, 256], P('kv', 'tp')
The draws below stay inside these ranges and needn't reach their ends.
All inputs are finite; a program needn't handle non-finite values.
Results may differ from the reference program's by a relative error of at most 0.03.
Values may be sent and summed in bfloat16 or wider, within the bound.
A program may use at most 64 MiB of HBM per device.

```python
import jax
import jax.numpy as jnp
from jax import lax

D = 4096
H = 16
DK = 128
DV = 256
FF = 16384
BATCH = 128
N_KV = 8
N_TP = 4


def draw_tokens(key, part):
    first, second = jax.random.split(key, 2)
    columns = jnp.exp(jnp.log(4.0) * (jnp.arange(D, dtype=jnp.float32) / D - 0.5))
    base = jax.random.normal(first, (BATCH, D), jnp.float32)
    rows = jnp.exp(jax.random.uniform(second, (BATCH, 1), jnp.float32, jnp.log(0.25), jnp.log(2.5)))
    return (base * rows * columns[None, :]).astype(jnp.bfloat16)


def place_ends(result, rng, low, top_value):
    longest = result.shape.index(max(result.shape))
    spots = []
    for shift in (0, 1):
        where = [jax.random.randint(jax.random.fold_in(rng, axis), (), 0, length) for axis, length in enumerate(result.shape)]
        where[longest] = (where[longest] + shift) % result.shape[longest]
        spots.append(tuple(where))
    return result.at[spots[0]].set(low).at[spots[1]].set(top_value)


def shard_levels(rng, extent, pieces, smallest, largest):
    def one(axis_at, blocks):
        steps = jax.random.uniform(jax.random.fold_in(jax.random.fold_in(rng, 6), axis_at), (blocks,), jnp.float32, smallest / len(pieces), largest / len(pieces))
        return jnp.repeat(jnp.exp(steps), extent[axis_at] // blocks).reshape((-1,) + (1,) * (len(extent) - axis_at - 1))

    gain = one(*pieces[0])
    for cut in pieces[1:]:
        gain = gain * one(*cut)
    return gain


def centred(rng, dims, scale, reach, pieces=(), kind=jnp.bfloat16):
    level = shard_levels(rng, dims, pieces, -0.22, 0.18) if pieces else 1.0
    array = jax.random.normal(rng, dims, jnp.float32) * scale * level
    return jnp.minimum(jnp.maximum(array, -reach), reach).astype(kind)


def setup_inputs(seed: int = 0) -> dict:
    seeds = jax.random.split(jax.random.key(seed), 14)
    tokens = draw_tokens(jax.random.fold_in(seeds[13], 71), 0)
    seq_pos = place_ends(jax.random.randint(seeds[1], (BATCH,), 0, 4096), jax.random.fold_in(seeds[1], 1), 0, 4095).astype(jnp.int32)
    state = centred(seeds[2], (BATCH, H, DK, DV), 0.1, 0.6, ((0, 8), (1, 4)), jnp.float32)
    norm_in_gain = jnp.clip(1.0 + 0.18 * jax.random.normal(seeds[3], (D,), jnp.float32), 0.1, 1.9)
    query_weight = centred(seeds[4], (D, H * DK), D ** -0.5, 0.09375, ((0, 8), (1, 4)))
    key_weight = centred(seeds[5], (D, H * DK), D ** -0.5, 0.09375, ((0, 8), (1, 4)))
    value_weight = centred(seeds[6], (D, H * DV), D ** -0.5, 0.09375, ((0, 8), (1, 4)))
    gate_weight = centred(seeds[7], (D, H * DV), D ** -0.5, 0.09375, ((0, 8), (1, 4)))
    head_gain = jnp.clip(1.0 + 0.18 * jax.random.normal(seeds[8], (H * DV,), jnp.float32), 0.1, 1.9)
    out_weight = centred(seeds[9], (H * DV, D), (H * DV) ** -0.5, 0.09375, ((0, 4), (1, 8)))
    norm_mlp_gain = jnp.clip(1.0 + 0.18 * jax.random.normal(seeds[10], (D,), jnp.float32), 0.1, 1.9)
    hidden_weight = centred(seeds[11], (D, FF), D ** -0.5, 0.09375, ((0, 8), (1, 4)))
    down_weight = centred(seeds[12], (FF, D), FF ** -0.5, 0.046875, ((0, 4), (1, 8)))
    return dict(tokens=tokens, seq_pos=seq_pos, state=state, norm_in_gain=norm_in_gain, query_weight=query_weight, key_weight=key_weight, value_weight=value_weight, gate_weight=gate_weight, head_gain=head_gain, out_weight=out_weight, norm_mlp_gain=norm_mlp_gain, hidden_weight=hidden_weight, down_weight=down_weight)


EPS = 1e-06

def rotate(vectors, positions):
    half = vectors.shape[-1] // 2
    inverse = jnp.power(10000.0, -jnp.arange(half, dtype=jnp.float32) / half)
    angles = positions.astype(jnp.float32)[:, None] * inverse[None, :]
    cosine = jnp.cos(angles)[:, None, :]
    sine = jnp.sin(angles)[:, None, :]
    first, second = (vectors[..., :half], vectors[..., half:])
    return jnp.concatenate([first * cosine - second * sine, first * sine + second * cosine], axis=-1)

def head_decay(head_ids):
    return 1.0 - jnp.exp2(-2.0 - 6.0 * head_ids / (H - 1))

def grouped_sum(left, right, groups):
    width = left.shape[1] // groups
    total = jnp.zeros((left.shape[0], right.shape[1]), jnp.float32)
    for group in range(groups):
        piece = jnp.dot(left[:, group * width:(group + 1) * width], right[group * width:(group + 1) * width], preferred_element_type=jnp.float32).astype(jnp.bfloat16)
        total = total + piece.astype(jnp.float32)
    return total

def reference(tokens, seq_pos, state, norm_in_gain, query_weight, key_weight, value_weight, gate_weight, head_gain, out_weight, norm_mlp_gain, hidden_weight, down_weight):
    batch = tokens.shape[0]
    tokens_f = tokens.astype(jnp.float32)
    scale_in = lax.rsqrt(lax.optimization_barrier(jnp.mean(tokens_f * tokens_f, axis=1)) + EPS)[:, None]
    normed_in = (tokens_f * norm_in_gain[None, :]).astype(jnp.bfloat16)
    query = grouped_sum(normed_in, query_weight, N_KV) * scale_in
    keys = grouped_sum(normed_in, key_weight, N_KV) * scale_in
    values = grouped_sum(normed_in, value_weight, N_KV) * scale_in
    gates = grouped_sum(normed_in, gate_weight, N_KV) * scale_in
    turned_query = rotate(query.reshape(batch, H, DK), seq_pos)
    turned_keys = rotate(keys.reshape(batch, H, DK), seq_pos) * DK ** (-0.5)
    decay = head_decay(jnp.arange(H, dtype=jnp.float32))
    new_state = decay[None, :, None, None] * state + jnp.einsum('bhk,bhv->bhkv', turned_keys, values.reshape(batch, H, DV), precision=lax.Precision.HIGHEST)
    read = jnp.einsum('bhk,bhkv->bhv', turned_query, new_state, precision=lax.Precision.HIGHEST)
    read = read * lax.rsqrt(lax.optimization_barrier(jnp.mean(read * read, axis=-1, keepdims=True)) + EPS)
    mixed = (read.reshape(batch, H * DV) * head_gain[None, :] * jax.nn.silu(gates)).astype(jnp.bfloat16)
    attn = grouped_sum(mixed, out_weight, N_TP)
    resid = (tokens_f + attn).astype(jnp.bfloat16)
    resid_f = resid.astype(jnp.float32)
    scale_mid = lax.rsqrt(lax.optimization_barrier(jnp.mean(resid_f * resid_f, axis=1)) + EPS)[:, None]
    normed_mid = (resid_f * norm_mlp_gain[None, :]).astype(jnp.bfloat16)
    hidden = grouped_sum(normed_mid, hidden_weight, N_KV) * scale_mid
    active = jnp.square(jax.nn.relu(hidden)).astype(jnp.bfloat16)
    down = grouped_sum(active, down_weight, N_TP)
    output = (resid_f + down).astype(jnp.bfloat16)
    return (output, new_state)
```

```python
import functools

import jax
import jax.numpy as jnp
from jax import lax
from jax.experimental import pallas as pl
from jax.experimental.pallas import tpu as pltpu
from jax.sharding import PartitionSpec as P

H = 16
DK = 128
DV = 256
EPS = 1e-06
MESH = pl.DeviceIdType.MESH
VMEM = pltpu.VMEM
DMA = pltpu.SemaphoreType.DMA


def remote(src, dst, send, recv, where):
    return pltpu.make_async_remote_copy(
        src_ref=src, dst_ref=dst, send_sem=send, recv_sem=recv, device_id=where, device_id_type=MESH
    )


def entry_barrier(n_kv, n_tp):
    barrier = pltpu.get_barrier_semaphore()
    for axis, n in (("kv", n_kv), ("tp", n_tp)):
        me = lax.axis_index(axis)
        for k in range(1, n):
            pl.semaphore_signal(
                barrier, inc=1, device_id={axis: lax.rem(me + k, n)}, device_id_type=MESH
            )
    pl.semaphore_wait(barrier, n_kv + n_tp - 2)


def gather_tp(own, rows, send, recv, n):
    me = lax.axis_index("tp")
    copies = [
        remote(own, rows.at[me], send.at[k], recv.at[k], {"tp": lax.rem(me + k, n)})
        for k in range(1, n)
    ]
    for copy in copies:
        copy.start()
    rows[me] = own[...]
    for copy in copies:
        copy.wait_recv()
    return copies


def reduce_tp(terms, landed, send, recv, n):
    me = lax.axis_index("tp")
    copies = []
    for k in range(1, n):
        to = lax.rem(me + k, n)
        copies.append(remote(terms.at[to], landed.at[k], send.at[k], recv.at[k], {"tp": to}))
    for copy in copies:
        copy.start()
    total = terms[me].astype(jnp.float32)
    for k, copy in enumerate(copies, 1):
        copy.wait_recv()
        total += landed[k].astype(jnp.float32)
    return total, copies


def squares_start(squares, landed, send, recv, n):
    me = lax.axis_index("kv")
    copies = []
    for k in range(1, n):
        to = lax.rem(me + k, n)
        copies.append(remote(squares.at[to], landed.at[k], send.at[k], recv.at[k], {"kv": to}))
    for copy in copies:
        copy.start()
    return copies


def squares_total(copies, squares, landed):
    total = squares[lax.axis_index("kv")]
    for k, copy in enumerate(copies, 1):
        copy.wait_recv()
        total += landed[k]
    return total[:, :1]


class Scatter:
    def __init__(self, terms, land_in, partial, land_out, sems, outer, inner):
        self.terms, self.land_in, self.partial, self.land_out = terms, land_in, partial, land_out
        me = lax.axis_index("kv")
        self.o, self.i = me // inner, lax.rem(me, inner)
        self.outer, self.inner = outer, inner
        send_in, recv_in, send_out, recv_out = sems
        self.first, self.second = {}, {}
        for s in self.order():
            to_o = lax.rem(self.o + s, outer)
            for k in range(1, inner):
                to_i = lax.rem(self.i + k, inner)
                self.first[s, k] = remote(
                    terms.at[to_o, to_i],
                    land_in.at[k, s],
                    send_in.at[k, s],
                    recv_in.at[k, s],
                    {"kv": self.o * inner + to_i},
                )
            if s:
                source = partial.at[s] if inner > 1 else terms.at[to_o, self.i]
                self.second[s] = remote(
                    source,
                    land_out.at[s],
                    send_out.at[s],
                    recv_out.at[s],
                    {"kv": to_o * inner + self.i},
                )

    def order(self):
        return list(range(1, self.outer)) + [0]

    def start(self):
        for copy in self.first.values():
            copy.start()

    def middle(self):
        for s in self.order():
            to_o = lax.rem(self.o + s, self.outer)
            if self.inner > 1:
                total = self.terms[to_o, self.i].astype(jnp.float32)
                for k in range(1, self.inner):
                    self.first[s, k].wait_recv()
                    total += self.land_in[k, s].astype(jnp.float32)
                self.partial[s] = total.astype(jnp.bfloat16)
            if s:
                self.second[s].start()

    def arrived(self):
        for copy in self.second.values():
            copy.wait_recv()

    def total(self, columns):
        if self.inner > 1:
            total = self.partial[0, :, columns].astype(jnp.float32)
        else:
            total = self.terms[self.o, self.i, :, columns].astype(jnp.float32)
        for s in range(1, self.outer):
            total += self.land_out[s, :, columns].astype(jnp.float32)
        return total

    def copies(self):
        return list(self.first.values()) + list(self.second.values())


class Gather:
    def __init__(self, held, sems, outer, inner):
        me = lax.axis_index("kv")
        o, i = me // inner, lax.rem(me, inner)
        send_out, recv_out, send_in, recv_in = sems
        self.outer, self.inner = outer, inner
        self.first, self.second = {}, {}
        for s in range(outer):
            if s:
                self.first[s] = remote(
                    held.at[o, i],
                    held.at[o, i],
                    send_out.at[s],
                    recv_out.at[s],
                    {"kv": lax.rem(o + s, outer) * inner + i},
                )
            origin = lax.rem(o + outer - s, outer)
            for k in range(1, inner):
                self.second[s, k] = remote(
                    held.at[origin, i],
                    held.at[origin, i],
                    send_in.at[k, s],
                    recv_in.at[k, s],
                    {"kv": o * inner + lax.rem(i + k, inner)},
                )

    def run(self):
        for copy in self.first.values():
            copy.start()
        for s in range(self.outer):
            if s:
                self.first[s].wait_recv()
            for k in range(1, self.inner):
                self.second[s, k].start()
        for copy in self.second.values():
            copy.wait_recv()

    def copies(self):
        return list(self.first.values()) + list(self.second.values())


def project_kernel(
    n_kv, n_tp, inner, features,
    tokens, gain, cosine, sine, wq, wk, wv, wg,
    qk_out, v_out, g_out,
    rows, weights, terms, land_in, partial, land_out, squares, squares_in,
    w_sem, tp_send, tp_recv, sq_send, sq_recv, s1, r1, s2, r2,
):
    outer = n_kv // inner
    own = cosine.shape[0]
    loads, offset = [], 0
    for index, ref in enumerate((wq, wk, wv, wg)):
        width = ref.shape[1]
        part = pl.ds(offset, width)
        loads.append((pltpu.make_async_copy(ref, weights.at[:, part], w_sem.at[index]), offset, width))
        offset += width
    for load, _, _ in loads:
        load.start()
    entry_barrier(n_kv, n_tp)
    pending = gather_tp(tokens, rows, tp_send, tp_recv, n_tp)
    batch = rows.shape[0] * rows.shape[1]
    x = rows[...].reshape(batch, rows.shape[2]).astype(jnp.float32)
    total = jnp.sum(x * x, axis=1, keepdims=True)
    squares[...] = jnp.broadcast_to(total, (batch, 128)).reshape(n_kv, own, 128)
    sq_copies = squares_start(squares, squares_in, sq_send, sq_recv, n_kv)
    normed = (x * gain[...]).astype(jnp.bfloat16)
    for load, offset, width in loads:
        load.wait()
        term = jnp.dot(
            normed, weights[:, offset : offset + width], preferred_element_type=jnp.float32
        ).astype(jnp.bfloat16)
        terms[:, :, :, offset : offset + width] = term.reshape(outer, inner, own, width)
    scatter = Scatter(terms, land_in, partial, land_out, (s1, r1, s2, r2), outer, inner)
    scatter.start()
    scatter.middle()
    scale = lax.rsqrt(squares_total(sq_copies, squares, squares_in) / features + EPS)
    scatter.arrived()
    c, s = cosine[...], sine[...]
    heads = wq.shape[1] // DK
    for h in range(2 * heads):
        vec = scatter.total(pl.ds(h * DK, DK)) * scale
        turned = vec * c + pltpu.roll(vec, DK // 2, 1) * s
        if h >= heads:
            turned = turned * DK ** (-0.5)
        qk_out[:, h, :] = turned
    for h in range(heads):
        v_out[:, h, :] = scatter.total(pl.ds(2 * heads * DK + h * DV, DV)) * scale
        g_out[:, h, :] = scatter.total(pl.ds(heads * (2 * DK + DV) + h * DV, DV)) * scale
    for copy in pending + sq_copies + scatter.copies():
        copy.wait_send()


def state_kernel(qk, v, g, gain, state, new_state, mixed, acc):
    heads = state.shape[1]
    b = pl.program_id(0)
    columns = qk[0].T
    first = lax.axis_index("tp") * heads
    for h in range(heads):
        ids = jnp.full((1, DV), first + h, jnp.int32).astype(jnp.float32)
        decay = 1.0 - jnp.exp2(-2.0 - 6.0 * ids / (H - 1))
        query = columns[:, h : h + 1]
        key = columns[:, heads + h : heads + h + 1]
        new = decay * state[0, h] + key * v[0, h : h + 1, :]
        new_state[0, h] = new
        read = jnp.sum(query * new, axis=0, keepdims=True)
        read = read * lax.rsqrt(jnp.mean(read * read, axis=-1, keepdims=True) + EPS)
        gate = g[0, h : h + 1, :]
        part = slice(h * DV, (h + 1) * DV)
        acc[pl.ds(b, 1), part] = read * gain[:, part] * (gate / (1.0 + jnp.exp(-gate)))

    @pl.when(b == pl.num_programs(0) - 1)
    def _():
        mixed[...] = acc[...].astype(jnp.bfloat16)


def mixer_kernel(
    n_kv, n_tp, inner, features, wide,
    mixed, tokens, gain, w_out, w_hidden, w_down,
    output,
    held, wo, wh, wd, out_terms, out_land, resid, rows, squares, squares_in,
    terms, land_in, partial, land_out, active, acc, down_terms, down_land,
    w_sem, gs1, gr1, gs2, gr2, os, orr, ts, tr, qs, qr, s1, r1, s2, r2, hs1, hr1, hs2, hr2, ds, dr,
):
    outer = n_kv // inner
    own, width = mixed.shape
    me = lax.axis_index("kv")
    loads = [
        pltpu.make_async_copy(w_out, wo, w_sem.at[0]),
        pltpu.make_async_copy(w_hidden, wh, w_sem.at[1]),
        pltpu.make_async_copy(w_down, wd, w_sem.at[2]),
    ]
    for load in loads:
        load.start()
    o, i = me // inner, lax.rem(me, inner)
    held[o, i] = mixed[...]
    entry_barrier(n_kv, n_tp)
    gather = Gather(held, (gs1, gr1, gs2, gr2), outer, inner)
    gather.run()
    pending = gather.copies()
    loads[0].wait()
    batch = n_kv * own
    piece = batch // n_tp
    cols = wo.shape[1]
    out_terms[...] = (
        jnp.dot(held[...].reshape(batch, width), wo[...], preferred_element_type=jnp.float32)
        .astype(jnp.bfloat16)
        .reshape(n_tp, piece, cols)
    )
    attn, copies = reduce_tp(out_terms, out_land, os, orr, n_tp)
    pending += copies
    resid[...] = (tokens[...].astype(jnp.float32) + attn).astype(jnp.bfloat16)
    pending += gather_tp(resid, rows, ts, tr, n_tp)
    x = rows[...].reshape(batch, cols).astype(jnp.float32)
    total = jnp.sum(x * x, axis=1, keepdims=True)
    squares[...] = jnp.broadcast_to(total, (batch, 128)).reshape(n_kv, own, 128)
    sq_copies = squares_start(squares, squares_in, qs, qr, n_kv)
    pending += sq_copies
    normed = (x * gain[...]).astype(jnp.bfloat16)
    loads[1].wait()
    hidden = wh.shape[1]

    @pl.loop(0, hidden // wide)
    def _(c):
        part = pl.ds(pl.multiple_of(c * wide, wide), wide)
        term = jnp.dot(normed, wh[:, part], preferred_element_type=jnp.float32)
        terms[:, :, :, part] = term.astype(jnp.bfloat16).reshape(outer, inner, own, wide)

    scatter = Scatter(terms, land_in, partial, land_out, (s1, r1, s2, r2), outer, inner)
    scatter.start()
    scatter.middle()
    scale = lax.rsqrt(squares_total(sq_copies, squares, squares_in) / features + EPS)
    scatter.arrived()
    pending += scatter.copies()
    for c in range(hidden // wide):
        part = pl.ds(c * wide, wide)
        value = jnp.maximum(scatter.total(part) * scale, 0.0)
        active[o, i, :, part] = (value * value).astype(jnp.bfloat16)
    gather = Gather(active, (hs1, hr1, hs2, hr2), outer, inner)
    gather.run()
    pending += gather.copies()
    loads[2].wait()
    acc[...] = jnp.zeros_like(acc)

    @pl.loop(0, hidden // wide)
    def _(c):
        part = pl.ds(pl.multiple_of(c * wide, wide), wide)
        left = active[:, :, :, part].reshape(batch, wide)
        acc[...] += jnp.dot(left, wd[part, :], preferred_element_type=jnp.float32)

    down_terms[...] = acc[...].astype(jnp.bfloat16).reshape(n_tp, piece, cols)
    down, copies = reduce_tp(down_terms, down_land, ds, dr, n_tp)
    pending += copies
    output[...] = (resid[...].astype(jnp.float32) + down).astype(jnp.bfloat16)
    for copy in pending:
        copy.wait_send()


def local(
    n_kv, n_tp, inner, features,
    tokens, seq_pos, state, norm_in_gain, query_weight, key_weight, value_weight, gate_weight,
    head_gain, out_weight, norm_mlp_gain, hidden_weight, down_weight,
):
    outer = n_kv // inner
    f32, bf16 = jnp.float32, jnp.bfloat16
    half = DK // 2
    inverse = jnp.power(10000.0, -jnp.arange(half, dtype=f32) / half)
    angles = seq_pos.astype(f32)[:, None] * inverse[None, :]
    cos, sin = jnp.cos(angles), jnp.sin(angles)
    cosine = jnp.concatenate([cos, cos], axis=1)
    sine = jnp.concatenate([-sin, sin], axis=1)

    own = seq_pos.shape[0]
    piece, cols = tokens.shape
    heads = state.shape[1]
    whole = heads * 2 * (DK + DV)
    vmem, hbm = pl.BlockSpec(memory_space=VMEM), pl.BlockSpec(memory_space=pl.ANY)

    def scatter_buffers(width):
        return [
            VMEM((outer, inner, own, width), bf16),
            VMEM((inner, outer, own, width), bf16),
            VMEM((outer, own, width), bf16),
            VMEM((outer, own, width), bf16),
        ]

    two_in = [DMA((inner, outer)), DMA((inner, outer))]
    two_out = [DMA((outer,)), DMA((outer,))]
    over_tp = [DMA((n_tp,)), DMA((n_tp,))]
    over_kv = [DMA((n_kv,)), DMA((n_kv,))]
    qk, v, g = pl.pallas_call(
        functools.partial(project_kernel, n_kv, n_tp, inner, features),
        out_shape=[
            jax.ShapeDtypeStruct((own, 2 * heads, DK), f32),
            jax.ShapeDtypeStruct((own, heads, DV), f32),
            jax.ShapeDtypeStruct((own, heads, DV), f32),
        ],
        in_specs=[vmem] * 4 + [hbm] * 4,
        out_specs=[vmem] * 3,
        scratch_shapes=[VMEM((n_tp, piece, cols), bf16), VMEM((cols, whole), bf16)]
        + scatter_buffers(whole)
        + [VMEM((n_kv, own, 128), f32), VMEM((n_kv, own, 128), f32), DMA((4,))]
        + over_tp + over_kv + two_in + two_out,
        compiler_params=pltpu.CompilerParams(
            collective_id=0, has_side_effects=True, vmem_limit_bytes=48 * 2**20
        ),
    )(
        tokens, norm_in_gain[None, :], cosine, sine,
        query_weight, key_weight, value_weight, gate_weight,
    )

    def per_row(*shape):
        return pl.BlockSpec((1,) + shape, lambda b: (b,) + (0,) * len(shape))

    new_state, mixed = pl.pallas_call(
        state_kernel,
        grid=(own,),
        out_shape=[
            jax.ShapeDtypeStruct(state.shape, f32),
            jax.ShapeDtypeStruct((own, heads * DV), bf16),
        ],
        in_specs=[
            per_row(2 * heads, DK),
            per_row(heads, DV),
            per_row(heads, DV),
            pl.BlockSpec((1, heads * DV), lambda b: (0, 0)),
            per_row(heads, DK, DV),
        ],
        out_specs=[per_row(heads, DK, DV), pl.BlockSpec((own, heads * DV), lambda b: (0, 0))],
        scratch_shapes=[VMEM((own, heads * DV), f32)],
    )(qk, v, g, head_gain[None, :], state)

    hidden = hidden_weight.shape[1]
    wide = min(512, hidden)
    output = pl.pallas_call(
        functools.partial(mixer_kernel, n_kv, n_tp, inner, features, wide),
        out_shape=jax.ShapeDtypeStruct(tokens.shape, bf16),
        in_specs=[vmem] * 3 + [hbm] * 3,
        out_specs=vmem,
        scratch_shapes=[
            VMEM((outer, inner, own, heads * DV), bf16),
            VMEM(out_weight.shape, bf16),
            VMEM(hidden_weight.shape, bf16),
            VMEM(down_weight.shape, bf16),
            VMEM((n_tp, piece, cols), bf16),
            VMEM((n_tp, piece, cols), bf16),
            VMEM((piece, cols), bf16),
            VMEM((n_tp, piece, cols), bf16),
            VMEM((n_kv, own, 128), f32),
            VMEM((n_kv, own, 128), f32),
        ]
        + scatter_buffers(hidden)
        + [
            VMEM((outer, inner, own, hidden), bf16),
            VMEM((n_tp * piece, cols), f32),
            VMEM((n_tp, piece, cols), bf16),
            VMEM((n_tp, piece, cols), bf16),
            DMA((3,)),
        ]
        + two_out + two_in
        + over_tp + over_tp + over_kv
        + two_in + two_out
        + two_out + two_in
        + over_tp,
        compiler_params=pltpu.CompilerParams(
            collective_id=1, has_side_effects=True, vmem_limit_bytes=48 * 2**20
        ),
    )(mixed, tokens, norm_mlp_gain[None, :], out_weight, hidden_weight, down_weight)
    return output, new_state


def inner_size(mesh):
    column = mesh.devices[:, 0] if mesh.axis_names[0] == "kv" else mesh.devices[0, :]
    heights = [getattr(device, "coords", (0, 0, at))[2] for at, device in enumerate(column)]
    count = 1
    while count < len(heights) and heights[count] == heights[0]:
        count += 1
    return count if len(heights) % count == 0 else 1


def solution(mesh):
    n_kv, n_tp = mesh.shape["kv"], mesh.shape["tp"]
    inner = inner_size(mesh)
    placed = (
        P("tp", "kv"), P("kv"), P("kv", "tp", None, None), P("kv"),
        P("kv", "tp"), P("kv", "tp"), P("kv", "tp"), P("kv", "tp"),
        P("tp"), P("tp", "kv"), P("kv"), P("kv", "tp"), P("tp", "kv"),
    )

    def step(*args):
        return local(n_kv, n_tp, inner, args[0].shape[1] * n_kv, *args)

    return jax.shard_map(
        step, mesh=mesh, in_specs=placed,
        out_specs=(P("tp", "kv"), P("kv", "tp", None, None)), check_vma=False,
    )
```

```python
import functools

import jax
import jax.numpy as jnp
from jax import lax
from jax.experimental import pallas as pl
from jax.experimental.pallas import tpu as pltpu
from jax.sharding import PartitionSpec as P

H = 16
DK = 128
DV = 256
EPS = 1e-06
MESH = pl.DeviceIdType.MESH
VMEM = pltpu.VMEM
DMA = pltpu.SemaphoreType.DMA


def remote(src, dst, send, recv, where):
    return pltpu.make_async_remote_copy(
        src_ref=src, dst_ref=dst, send_sem=send, recv_sem=recv, device_id=where, device_id_type=MESH
    )


def entry_barrier(n_kv, n_tp):
    barrier = pltpu.get_barrier_semaphore()
    for axis, n in (("kv", n_kv), ("tp", n_tp)):
        me = lax.axis_index(axis)
        for k in range(1, n):
            pl.semaphore_signal(
                barrier, inc=1, device_id={axis: lax.rem(me + k, n)}, device_id_type=MESH
            )
    pl.semaphore_wait(barrier, n_kv + n_tp - 2)


def gather_tp(own, rows, send, recv, n):
    me = lax.axis_index("tp")
    copies = [
        remote(own, rows.at[me], send.at[k], recv.at[k], {"tp": lax.rem(me + k, n)})
        for k in range(1, n)
    ]
    for copy in copies:
        copy.start()
    rows[me] = own[...]
    for copy in copies:
        copy.wait_recv()
    return copies


def reduce_tp(terms, landed, send, recv, n):
    me = lax.axis_index("tp")
    copies = []
    for k in range(1, n):
        to = lax.rem(me + k, n)
        copies.append(remote(terms.at[to], landed.at[k], send.at[k], recv.at[k], {"tp": to}))
    for copy in copies:
        copy.start()
    total = terms[me].astype(jnp.float32)
    for k, copy in enumerate(copies, 1):
        copy.wait_recv()
        total += landed[k].astype(jnp.float32)
    return total, copies


def squares_start(squares, landed, send, recv, n):
    me = lax.axis_index("kv")
    copies = []
    for k in range(1, n):
        to = lax.rem(me + k, n)
        copies.append(remote(squares.at[to], landed.at[k], send.at[k], recv.at[k], {"kv": to}))
    for copy in copies:
        copy.start()
    return copies


def squares_total(copies, squares, landed):
    total = squares[lax.axis_index("kv")]
    for k, copy in enumerate(copies, 1):
        copy.wait_recv()
        total += landed[k]
    return total[:, :1]


class Scatter:
    def __init__(self, terms, land_in, partial, land_out, sems, outer, inner):
        self.terms, self.land_in, self.partial, self.land_out = terms, land_in, partial, land_out
        me = lax.axis_index("kv")
        self.o, self.i = me // inner, lax.rem(me, inner)
        self.outer, self.inner = outer, inner
        send_in, recv_in, send_out, recv_out = sems
        self.first, self.second = {}, {}
        for s in self.order():
            to_o = lax.rem(self.o + s, outer)
            for k in range(1, inner):
                to_i = lax.rem(self.i + k, inner)
                self.first[s, k] = remote(
                    terms.at[to_o, to_i],
                    land_in.at[k, s],
                    send_in.at[k, s],
                    recv_in.at[k, s],
                    {"kv": self.o * inner + to_i},
                )
            if s:
                source = partial.at[s] if inner > 1 else terms.at[to_o, self.i]
                self.second[s] = remote(
                    source,
                    land_out.at[s],
                    send_out.at[s],
                    recv_out.at[s],
                    {"kv": to_o * inner + self.i},
                )

    def order(self):
        return list(range(1, self.outer)) + [0]

    def start(self):
        for copy in self.first.values():
            copy.start()

    def middle(self):
        for s in self.order():
            to_o = lax.rem(self.o + s, self.outer)
            if self.inner > 1:
                total = self.terms[to_o, self.i].astype(jnp.float32)
                for k in range(1, self.inner):
                    self.first[s, k].wait_recv()
                    total += self.land_in[k, s].astype(jnp.float32)
                self.partial[s] = total.astype(jnp.bfloat16)
            if s:
                self.second[s].start()

    def arrived(self):
        for copy in self.second.values():
            copy.wait_recv()

    def total(self, columns):
        if self.inner > 1:
            total = self.partial[0, :, columns].astype(jnp.float32)
        else:
            total = self.terms[self.o, self.i, :, columns].astype(jnp.float32)
        for s in range(1, self.outer):
            total += self.land_out[s, :, columns].astype(jnp.float32)
        return total

    def copies(self):
        return list(self.first.values()) + list(self.second.values())


class Gather:
    def __init__(self, held, sems, outer, inner):
        me = lax.axis_index("kv")
        o, i = me // inner, lax.rem(me, inner)
        send_out, recv_out, send_in, recv_in = sems
        self.outer, self.inner = outer, inner
        self.first, self.second = {}, {}
        for s in range(outer):
            if s:
                self.first[s] = remote(
                    held.at[o, i],
                    held.at[o, i],
                    send_out.at[s],
                    recv_out.at[s],
                    {"kv": lax.rem(o + s, outer) * inner + i},
                )
            origin = lax.rem(o + outer - s, outer)
            for k in range(1, inner):
                self.second[s, k] = remote(
                    held.at[origin, i],
                    held.at[origin, i],
                    send_in.at[k, s],
                    recv_in.at[k, s],
                    {"kv": o * inner + lax.rem(i + k, inner)},
                )

    def run(self):
        for copy in self.first.values():
            copy.start()
        for s in range(self.outer):
            if s:
                self.first[s].wait_recv()
            for k in range(1, self.inner):
                self.second[s, k].start()
        for copy in self.second.values():
            copy.wait_recv()

    def copies(self):
        return list(self.first.values()) + list(self.second.values())


def layer_kernel(
    n_kv, n_tp, inner, features, wide,
    cosine, sine, tokens_hbm, gain_hbm, mid_gain_hbm, head_gain_hbm,
    wq, wk, wv, wg, w_out, w_hidden, w_down, state,
    output, new_state,
    tokens, gain, mid_gain, head_gain,
    rows, weights, terms, land_in, partial, land_out, squares, squares_in, qk, values, gates, mixed,
    held, wo, wh, wd, out_terms, out_land, resid, rows_mid, squares_mid, squares_mid_in,
    terms_h, land_in_h, partial_h, land_out_h, active, acc, down_terms, down_land,
    small_sem, w_sem, state_sem,
    tp_send, tp_recv, sq_send, sq_recv, s1, r1, s2, r2,
    gs1, gr1, gs2, gr2, os, orr, ts, tr, qs, qr, hs1, hr1, hs2, hr2, as1, ar1, as2, ar2, ds, dr,
):
    outer = n_kv // inner
    own = cosine.shape[0]
    me = lax.axis_index("kv")
    o, i = me // inner, lax.rem(me, inner)
    small = [
        pltpu.make_async_copy(src, dst, small_sem.at[at])
        for at, (src, dst) in enumerate(
            (
                (tokens_hbm, tokens),
                (gain_hbm, gain),
                (mid_gain_hbm, mid_gain),
                (head_gain_hbm, head_gain),
            )
        )
    ]
    for load in small:
        load.start()
    loads, offset = [], 0
    for index, ref in enumerate((wq, wk, wv, wg)):
        width = ref.shape[1]
        part = pl.ds(offset, width)
        loads.append((pltpu.make_async_copy(ref, weights.at[:, part], w_sem.at[index]), offset, width))
        offset += width
    for load, _, _ in loads:
        load.start()
    late = [
        pltpu.make_async_copy(w_out, wo, w_sem.at[4]),
        pltpu.make_async_copy(w_hidden, wh, w_sem.at[5]),
        pltpu.make_async_copy(w_down, wd, w_sem.at[6]),
    ]
    state_load = pltpu.make_async_copy(state, new_state, state_sem.at[0])
    entry_barrier(n_kv, n_tp)
    for load in small:
        load.wait()
    pending = gather_tp(tokens, rows, tp_send, tp_recv, n_tp)
    batch = rows.shape[0] * rows.shape[1]
    piece, cols = tokens.shape
    x = rows[...].reshape(batch, cols).astype(jnp.float32)
    total = jnp.sum(x * x, axis=1, keepdims=True)
    squares[...] = jnp.broadcast_to(total, (batch, 128)).reshape(n_kv, own, 128)
    sq_copies = squares_start(squares, squares_in, sq_send, sq_recv, n_kv)
    normed = (x * gain[...]).astype(jnp.bfloat16)
    for load, offset, width in loads:
        load.wait()
        term = jnp.dot(
            normed, weights[:, offset : offset + width], preferred_element_type=jnp.float32
        ).astype(jnp.bfloat16)
        terms[:, :, :, offset : offset + width] = term.reshape(outer, inner, own, width)
    scatter = Scatter(terms, land_in, partial, land_out, (s1, r1, s2, r2), outer, inner)
    scatter.start()
    state_load.start()
    for load in late:
        load.start()
    scatter.middle()
    scale = lax.rsqrt(squares_total(sq_copies, squares, squares_in) / features + EPS)
    scatter.arrived()
    c, s = cosine[...], sine[...]
    heads = wq.shape[1] // DK
    for h in range(2 * heads):
        vec = scatter.total(pl.ds(h * DK, DK)) * scale
        turned = vec * c + pltpu.roll(vec, DK // 2, 1) * s
        if h >= heads:
            turned = turned * DK ** (-0.5)
        qk[:, h, :] = turned
    for h in range(heads):
        values[:, h, :] = scatter.total(pl.ds(2 * heads * DK + h * DV, DV)) * scale
        gates[:, h, :] = scatter.total(pl.ds(heads * (2 * DK + DV) + h * DV, DV)) * scale
    pending += sq_copies + scatter.copies()
    first = lax.axis_index("tp") * heads
    state_load.wait()

    @pl.loop(0, own)
    def _(b):
        columns = qk[b].T
        v, g = values[b], gates[b]
        for h in range(heads):
            ids = jnp.full((1, DV), first + h, jnp.int32).astype(jnp.float32)
            decay = 1.0 - jnp.exp2(-2.0 - 6.0 * ids / (heads * n_tp - 1))
            query = columns[:, h : h + 1]
            key = columns[:, heads + h : heads + h + 1]
            new = decay * new_state[b, h] + key * v[h : h + 1, :]
            new_state[b, h] = new
            read = jnp.sum(query * new, axis=0, keepdims=True)
            read = read * lax.rsqrt(jnp.mean(read * read, axis=-1, keepdims=True) + EPS)
            gate = g[h : h + 1, :]
            part = slice(h * DV, (h + 1) * DV)
            mixed[pl.ds(b, 1), part] = read * head_gain[:, part] * (gate / (1.0 + jnp.exp(-gate)))

    held[o, i] = mixed[...].astype(jnp.bfloat16)
    gather = Gather(held, (gs1, gr1, gs2, gr2), outer, inner)
    gather.run()
    pending += gather.copies()
    late[0].wait()
    out_terms[...] = (
        jnp.dot(
            held[...].reshape(batch, mixed.shape[1]), wo[...], preferred_element_type=jnp.float32
        )
        .astype(jnp.bfloat16)
        .reshape(n_tp, piece, cols)
    )
    attn, copies = reduce_tp(out_terms, out_land, os, orr, n_tp)
    pending += copies
    resid[...] = (tokens[...].astype(jnp.float32) + attn).astype(jnp.bfloat16)
    pending += gather_tp(resid, rows_mid, ts, tr, n_tp)
    x = rows_mid[...].reshape(batch, cols).astype(jnp.float32)
    total = jnp.sum(x * x, axis=1, keepdims=True)
    squares_mid[...] = jnp.broadcast_to(total, (batch, 128)).reshape(n_kv, own, 128)
    sq_copies = squares_start(squares_mid, squares_mid_in, qs, qr, n_kv)
    pending += sq_copies
    normed = (x * mid_gain[...]).astype(jnp.bfloat16)
    late[1].wait()
    hidden = wh.shape[1]

    @pl.loop(0, hidden // wide)
    def _(c):
        part = pl.ds(pl.multiple_of(c * wide, wide), wide)
        term = jnp.dot(normed, wh[:, part], preferred_element_type=jnp.float32)
        terms_h[:, :, :, part] = term.astype(jnp.bfloat16).reshape(outer, inner, own, wide)

    scatter = Scatter(terms_h, land_in_h, partial_h, land_out_h, (hs1, hr1, hs2, hr2), outer, inner)
    scatter.start()
    scatter.middle()
    scale = lax.rsqrt(squares_total(sq_copies, squares_mid, squares_mid_in) / features + EPS)
    scatter.arrived()
    pending += scatter.copies()
    for c in range(hidden // wide):
        part = pl.ds(c * wide, wide)
        value = jnp.maximum(scatter.total(part) * scale, 0.0)
        active[o, i, :, part] = (value * value).astype(jnp.bfloat16)
    gather = Gather(active, (as1, ar1, as2, ar2), outer, inner)
    gather.run()
    pending += gather.copies()
    late[2].wait()
    acc[...] = jnp.zeros_like(acc)

    @pl.loop(0, hidden // wide)
    def _(c):
        part = pl.ds(pl.multiple_of(c * wide, wide), wide)
        left = active[:, :, :, part].reshape(batch, wide)
        acc[...] += jnp.dot(left, wd[part, :], preferred_element_type=jnp.float32)

    down_terms[...] = acc[...].astype(jnp.bfloat16).reshape(n_tp, piece, cols)
    down, copies = reduce_tp(down_terms, down_land, ds, dr, n_tp)
    pending += copies
    output[...] = (resid[...].astype(jnp.float32) + down).astype(jnp.bfloat16)
    for copy in pending:
        copy.wait_send()


def local(
    n_kv, n_tp, inner, features,
    tokens, seq_pos, state, norm_in_gain, query_weight, key_weight, value_weight, gate_weight,
    head_gain, out_weight, norm_mlp_gain, hidden_weight, down_weight,
):
    outer = n_kv // inner
    f32, bf16 = jnp.float32, jnp.bfloat16
    half = DK // 2
    inverse = jnp.power(10000.0, -jnp.arange(half, dtype=f32) / half)
    angles = seq_pos.astype(f32)[:, None] * inverse[None, :]
    cos, sin = jnp.cos(angles), jnp.sin(angles)
    cosine = jnp.concatenate([cos, cos], axis=1)
    sine = jnp.concatenate([-sin, sin], axis=1)

    own = seq_pos.shape[0]
    piece, cols = tokens.shape
    heads = state.shape[1]
    whole = heads * 2 * (DK + DV)
    hidden = hidden_weight.shape[1]
    wide = min(512, hidden)
    vmem, hbm = pl.BlockSpec(memory_space=VMEM), pl.BlockSpec(memory_space=pltpu.HBM)

    def scatter_buffers(width):
        return [
            VMEM((outer, inner, own, width), bf16),
            VMEM((inner, outer, own, width), bf16),
            VMEM((outer, own, width), bf16),
            VMEM((outer, own, width), bf16),
        ]

    two_in = [DMA((inner, outer)), DMA((inner, outer))]
    two_out = [DMA((outer,)), DMA((outer,))]
    over_tp = [DMA((n_tp,)), DMA((n_tp,))]
    over_kv = [DMA((n_kv,)), DMA((n_kv,))]
    squares = [VMEM((n_kv, own, 128), f32), VMEM((n_kv, own, 128), f32)]
    tp_rows = VMEM((n_tp, piece, cols), bf16)
    return pl.pallas_call(
        functools.partial(layer_kernel, n_kv, n_tp, inner, features, wide),
        out_shape=[
            jax.ShapeDtypeStruct(tokens.shape, bf16),
            jax.ShapeDtypeStruct(state.shape, f32),
        ],
        in_specs=[vmem] * 2 + [hbm] * 12,
        out_specs=[vmem] * 2,
        scratch_shapes=[
            VMEM(tokens.shape, bf16), VMEM((1, cols), f32), VMEM((1, cols), f32),
            VMEM((1, heads * DV), f32),
            tp_rows, VMEM((cols, whole), bf16),
        ]
        + scatter_buffers(whole)
        + squares
        + [
            VMEM((own, 2 * heads, DK), f32),
            VMEM((own, heads, DV), f32),
            VMEM((own, heads, DV), f32),
            VMEM((own, heads * DV), f32),
            VMEM((outer, inner, own, heads * DV), bf16),
            VMEM(out_weight.shape, bf16),
            VMEM(hidden_weight.shape, bf16),
            VMEM(down_weight.shape, bf16),
            tp_rows, tp_rows, VMEM((piece, cols), bf16), tp_rows,
        ]
        + squares
        + scatter_buffers(hidden)
        + [
            VMEM((outer, inner, own, hidden), bf16),
            VMEM((n_tp * piece, cols), f32),
            tp_rows, tp_rows,
            DMA((4,)), DMA((7,)), DMA((1,)),
        ]
        + over_tp + over_kv + two_in + two_out
        + two_out + two_in
        + over_tp + over_tp + over_kv
        + two_in + two_out
        + two_out + two_in
        + over_tp,
        compiler_params=pltpu.CompilerParams(
            collective_id=0, has_side_effects=True, vmem_limit_bytes=48 * 2**20
        ),
    )(
        cosine, sine, tokens, norm_in_gain[None, :], norm_mlp_gain[None, :], head_gain[None, :],
        query_weight, key_weight, value_weight, gate_weight,
        out_weight, hidden_weight, down_weight, state,
    )


def inner_size(mesh):
    column = mesh.devices[:, 0] if mesh.axis_names[0] == "kv" else mesh.devices[0, :]
    heights = [getattr(device, "coords", (0, 0, at))[2] for at, device in enumerate(column)]
    count = 1
    while count < len(heights) and heights[count] == heights[0]:
        count += 1
    return count if len(heights) % count == 0 else 1


def solution(mesh):
    n_kv, n_tp = mesh.shape["kv"], mesh.shape["tp"]
    inner = inner_size(mesh)
    placed = (
        P("tp", "kv"), P("kv"), P("kv", "tp", None, None), P("kv"),
        P("kv", "tp"), P("kv", "tp"), P("kv", "tp"), P("kv", "tp"),
        P("tp"), P("tp", "kv"), P("kv"), P("kv", "tp"), P("tp", "kv"),
    )

    def step(*args):
        return local(n_kv, n_tp, inner, args[0].shape[1] * n_kv, *args)

    return jax.shard_map(
        step, mesh=mesh, in_specs=placed,
        out_specs=(P("tp", "kv"), P("kv", "tp", None, None)), check_vma=False,
    )
```

```python
import functools

import jax
import jax.numpy as jnp
from jax import lax
from jax.experimental import pallas as pl
from jax.experimental.pallas import tpu as pltpu
from jax.sharding import PartitionSpec as P

H = 16
DK = 128
DV = 256
EPS = 1e-06
CHUNKS = 2
MESH = pl.DeviceIdType.MESH
VMEM = pltpu.VMEM
DMA = pltpu.SemaphoreType.DMA


def remote(src, dst, send, recv, where):
    return pltpu.make_async_remote_copy(
        src_ref=src, dst_ref=dst, send_sem=send, recv_sem=recv, device_id=where, device_id_type=MESH
    )


def entry_barrier(n_kv, n_tp):
    barrier = pltpu.get_barrier_semaphore()
    for axis, n in (("kv", n_kv), ("tp", n_tp)):
        me = lax.axis_index(axis)
        for k in range(1, n):
            pl.semaphore_signal(
                barrier, inc=1, device_id={axis: lax.rem(me + k, n)}, device_id_type=MESH
            )
    pl.semaphore_wait(barrier, n_kv + n_tp - 2)


def gather_tp(own, rows, send, recv, n):
    me = lax.axis_index("tp")
    copies = [
        remote(own, rows.at[me], send.at[k], recv.at[k], {"tp": lax.rem(me + k, n)})
        for k in range(1, n)
    ]
    for copy in copies:
        copy.start()
    rows[me] = own[...]
    for copy in copies:
        copy.wait_recv()
    return copies


def reduce_tp(terms, landed, send, recv, n):
    me = lax.axis_index("tp")
    copies = []
    for k in range(1, n):
        to = lax.rem(me + k, n)
        copies.append(remote(terms.at[to], landed.at[k], send.at[k], recv.at[k], {"tp": to}))
    for copy in copies:
        copy.start()
    total = terms[me].astype(jnp.float32)
    for k, copy in enumerate(copies, 1):
        copy.wait_recv()
        total += landed[k].astype(jnp.float32)
    return total, copies


def squares_start(squares, landed, send, recv, n):
    me = lax.axis_index("kv")
    copies = []
    for k in range(1, n):
        to = lax.rem(me + k, n)
        copies.append(remote(squares.at[to], landed.at[k], send.at[k], recv.at[k], {"kv": to}))
    for copy in copies:
        copy.start()
    return copies


def squares_total(copies, squares, landed):
    total = squares[lax.axis_index("kv")]
    for k, copy in enumerate(copies, 1):
        copy.wait_recv()
        total += landed[k]
    return total[:, :1]


class Scatter:
    def __init__(self, terms, land_in, partial, land_out, sems, outer, inner):
        self.terms, self.land_in, self.partial, self.land_out = terms, land_in, partial, land_out
        me = lax.axis_index("kv")
        self.o, self.i = me // inner, lax.rem(me, inner)
        self.outer, self.inner = outer, inner
        send_in, recv_in, send_out, recv_out = sems
        self.first, self.second = {}, {}
        for s in self.order():
            to_o = lax.rem(self.o + s, outer)
            for k in range(1, inner):
                to_i = lax.rem(self.i + k, inner)
                self.first[s, k] = remote(
                    terms.at[to_o, to_i],
                    land_in.at[k, s],
                    send_in.at[k, s],
                    recv_in.at[k, s],
                    {"kv": self.o * inner + to_i},
                )
            if s:
                source = partial.at[s] if inner > 1 else terms.at[to_o, self.i]
                self.second[s] = remote(
                    source,
                    land_out.at[s],
                    send_out.at[s],
                    recv_out.at[s],
                    {"kv": to_o * inner + self.i},
                )

    def order(self):
        return list(range(1, self.outer)) + [0]

    def start(self):
        for copy in self.first.values():
            copy.start()

    def middle(self):
        for s in self.order():
            to_o = lax.rem(self.o + s, self.outer)
            if self.inner > 1:
                total = self.terms[to_o, self.i].astype(jnp.float32)
                for k in range(1, self.inner):
                    self.first[s, k].wait_recv()
                    total += self.land_in[k, s].astype(jnp.float32)
                self.partial[s] = total.astype(jnp.bfloat16)
            if s:
                self.second[s].start()

    def arrived(self):
        for copy in self.second.values():
            copy.wait_recv()

    def total(self, columns):
        if self.inner > 1:
            total = self.partial[0, :, columns].astype(jnp.float32)
        else:
            total = self.terms[self.o, self.i, :, columns].astype(jnp.float32)
        for s in range(1, self.outer):
            total += self.land_out[s, :, columns].astype(jnp.float32)
        return total

    def copies(self):
        return list(self.first.values()) + list(self.second.values())


class Gather:
    def __init__(self, held, sems, outer, inner):
        me = lax.axis_index("kv")
        o, i = me // inner, lax.rem(me, inner)
        send_out, recv_out, send_in, recv_in = sems
        self.outer, self.inner = outer, inner
        self.first, self.second = {}, {}
        for s in range(outer):
            if s:
                self.first[s] = remote(
                    held.at[o, i],
                    held.at[o, i],
                    send_out.at[s],
                    recv_out.at[s],
                    {"kv": lax.rem(o + s, outer) * inner + i},
                )
            origin = lax.rem(o + outer - s, outer)
            for k in range(1, inner):
                self.second[s, k] = remote(
                    held.at[origin, i],
                    held.at[origin, i],
                    send_in.at[k, s],
                    recv_in.at[k, s],
                    {"kv": o * inner + lax.rem(i + k, inner)},
                )

    def start(self):
        for copy in self.first.values():
            copy.start()

    def forward(self):
        for s in range(self.outer):
            if s:
                self.first[s].wait_recv()
            for k in range(1, self.inner):
                self.second[s, k].start()

    def arrived(self):
        for copy in self.second.values():
            copy.wait_recv()

    def copies(self):
        return list(self.first.values()) + list(self.second.values())


def layer_kernel(
    n_kv, n_tp, inner, features, wide,
    cosine, sine, tokens_hbm, gain_hbm, mid_gain_hbm, head_gain_hbm,
    wq, wk, wv, wg, w_out, w_hidden, w_down, state,
    output, new_state,
    tokens, gain, mid_gain, head_gain,
    rows, weights, terms, land_in, partial, land_out, g_terms, g_land_in, g_partial, g_land_out,
    squares, squares_in, qk, values, mixed, held_state, fresh, columns,
    held, wo, wh, wd, out_terms, out_land, resid, rows_mid, squares_mid, squares_mid_in,
    terms_h, land_in_h, partial_h, land_out_h, active, acc, down_terms, down_land,
    small_sem, w_sem, state_sem,
    tp_send, tp_recv, sq_send, sq_recv, s1, r1, s2, r2, t1, u1, t2, u2,
    gs1, gr1, gs2, gr2, os, orr, ts, tr, qs, qr, hs1, hr1, hs2, hr2, as1, ar1, as2, ar2, ds, dr,
):
    outer = n_kv // inner
    own = cosine.shape[0]
    me = lax.axis_index("kv")
    o, i = me // inner, lax.rem(me, inner)
    small = [
        pltpu.make_async_copy(src, dst, small_sem.at[at])
        for at, (src, dst) in enumerate(
            (
                (tokens_hbm, tokens),
                (gain_hbm, gain),
                (mid_gain_hbm, mid_gain),
                (head_gain_hbm, head_gain),
            )
        )
    ]
    for load in small:
        load.start()
    loads, offset = [], 0
    for index, ref in enumerate((wq, wk, wv, wg)):
        width = ref.shape[1]
        part = pl.ds(offset, width)
        loads.append((pltpu.make_async_copy(ref, weights.at[:, part], w_sem.at[index]), offset, width))
        offset += width
    for load, _, _ in loads:
        load.start()
    late = [
        pltpu.make_async_copy(w_out, wo, w_sem.at[4]),
        pltpu.make_async_copy(w_hidden, wh, w_sem.at[5]),
        pltpu.make_async_copy(w_down, wd, w_sem.at[6]),
    ]
    state_load = pltpu.make_async_copy(state, held_state, state_sem.at[0])
    entry_barrier(n_kv, n_tp)
    for load in small:
        load.wait()
    pending = gather_tp(tokens, rows, tp_send, tp_recv, n_tp)
    batch = rows.shape[0] * rows.shape[1]
    piece, cols = tokens.shape
    x = rows[...].reshape(batch, cols).astype(jnp.float32)
    total = jnp.sum(x * x, axis=1, keepdims=True)
    squares[...] = jnp.broadcast_to(total, (batch, 128)).reshape(n_kv, own, 128)
    sq_copies = squares_start(squares, squares_in, sq_send, sq_recv, n_kv)
    normed = (x * gain[...]).astype(jnp.bfloat16)
    scatter = Scatter(terms, land_in, partial, land_out, (s1, r1, s2, r2), outer, inner)
    gating = Scatter(g_terms, g_land_in, g_partial, g_land_out, (t1, u1, t2, u2), outer, inner)
    for index, (load, offset, width) in enumerate(loads):
        load.wait()
        term = jnp.dot(
            normed, weights[:, offset : offset + width], preferred_element_type=jnp.float32
        ).astype(jnp.bfloat16)
        if index < 3:
            terms[:, :, :, offset : offset + width] = term.reshape(outer, inner, own, width)
        else:
            g_terms[...] = term.reshape(outer, inner, own, width)
        if index == 2:
            scatter.start()
    gating.start()
    state_load.start()
    for load in late:
        load.start()
    scatter.middle()
    gating.middle()
    scale = lax.rsqrt(squares_total(sq_copies, squares, squares_in) / features + EPS)
    scatter.arrived()
    c, s = cosine[...], sine[...]
    heads = wq.shape[1] // DK
    for h in range(2 * heads):
        vec = scatter.total(pl.ds(h * DK, DK)) * scale
        turned = vec * c + pltpu.roll(vec, DK // 2, 1) * s
        if h >= heads:
            turned = turned * DK ** (-0.5)
        qk[:, h, :] = turned
    for h in range(heads):
        values[:, h, :] = scatter.total(pl.ds(2 * heads * DK + h * DV, DV)) * scale
    pending += sq_copies + scatter.copies() + gating.copies()
    first = lax.axis_index("tp") * heads
    state_load.wait()

    decays = []
    for h in range(heads):
        ids = jnp.full((1, DV), first + h, jnp.int32).astype(jnp.float32)
        decays.append(1.0 - jnp.exp2(-2.0 - 6.0 * ids / (heads * n_tp - 1)))
    for b in range(own):
        columns[b] = qk[b].T

    @pl.loop(0, own, unroll=2)
    def _(b):
        for h in range(heads):
            query = columns[b, :, h : h + 1]
            key = columns[b, :, heads + h : heads + h + 1]
            new = decays[h] * held_state[b, h] + key * values[b, h : h + 1, :]
            fresh[b, h] = new
            mixed[pl.ds(b, 1), h * DV : (h + 1) * DV] = jnp.sum(query * new, axis=0, keepdims=True)

    state_store = pltpu.make_async_copy(fresh, new_state, state_sem.at[1])
    state_store.start()
    gating.arrived()
    for h in range(heads):
        part = pl.ds(h * DV, DV)
        gate = gating.total(part) * scale
        read = mixed[:, part]
        read = read * lax.rsqrt(jnp.mean(read * read, axis=-1, keepdims=True) + EPS)
        value = read * head_gain[:, part] * (gate / (1.0 + jnp.exp(-gate)))
        held[o, i, :, part] = value.astype(jnp.bfloat16)
    gather = Gather(held, (gs1, gr1, gs2, gr2), outer, inner)
    gather.start()
    gather.forward()
    gather.arrived()
    pending += gather.copies()
    late[0].wait()
    out_terms[...] = (
        jnp.dot(
            held[...].reshape(batch, mixed.shape[1]), wo[...], preferred_element_type=jnp.float32
        )
        .astype(jnp.bfloat16)
        .reshape(n_tp, piece, cols)
    )
    attn, copies = reduce_tp(out_terms, out_land, os, orr, n_tp)
    pending += copies
    resid[...] = (tokens[...].astype(jnp.float32) + attn).astype(jnp.bfloat16)
    pending += gather_tp(resid, rows_mid, ts, tr, n_tp)
    x = rows_mid[...].reshape(batch, cols).astype(jnp.float32)
    total = jnp.sum(x * x, axis=1, keepdims=True)
    squares_mid[...] = jnp.broadcast_to(total, (batch, 128)).reshape(n_kv, own, 128)
    sq_copies = squares_start(squares_mid, squares_mid_in, qs, qr, n_kv)
    pending += sq_copies
    normed = (x * mid_gain[...]).astype(jnp.bfloat16)
    late[1].wait()
    hidden = wh.shape[1]

    steps = hidden // CHUNKS // wide
    scatters, gathers = [], []
    for chunk in range(CHUNKS):

        @pl.loop(0, steps)
        def _(c):
            here = pl.ds(pl.multiple_of((chunk * steps + c) * wide, wide), wide)
            part = pl.ds(pl.multiple_of(c * wide, wide), wide)
            term = jnp.dot(normed, wh[:, here], preferred_element_type=jnp.float32)
            terms_h[chunk, :, :, :, part] = term.astype(jnp.bfloat16).reshape(
                outer, inner, own, wide
            )

        scatter = Scatter(
            terms_h.at[chunk], land_in_h.at[chunk], partial_h.at[chunk], land_out_h.at[chunk],
            [sem.at[chunk] for sem in (hs1, hr1, hs2, hr2)], outer, inner,
        )
        scatter.start()
        scatters.append(scatter)
    for scatter in scatters:
        scatter.middle()
    scale = lax.rsqrt(squares_total(sq_copies, squares_mid, squares_mid_in) / features + EPS)
    for chunk, scatter in enumerate(scatters):
        scatter.arrived()
        pending += scatter.copies()
        for c in range(steps):
            part = pl.ds(c * wide, wide)
            value = jnp.maximum(scatter.total(part) * scale, 0.0)
            active[chunk, o, i, :, part] = (value * value).astype(jnp.bfloat16)
        gather = Gather(
            active.at[chunk], [sem.at[chunk] for sem in (as1, ar1, as2, ar2)], outer, inner
        )
        gather.start()
        gathers.append(gather)
    for gather in gathers:
        gather.forward()
    late[2].wait()
    acc[...] = jnp.zeros_like(acc)
    for chunk, gather in enumerate(gathers):
        gather.arrived()
        pending += gather.copies()

        @pl.loop(0, steps)
        def _(c):
            here = pl.ds(pl.multiple_of((chunk * steps + c) * wide, wide), wide)
            part = pl.ds(pl.multiple_of(c * wide, wide), wide)
            left = active[chunk, :, :, :, part].reshape(batch, wide)
            acc[...] += jnp.dot(left, wd[here, :], preferred_element_type=jnp.float32)

    down_terms[...] = acc[...].astype(jnp.bfloat16).reshape(n_tp, piece, cols)
    down, copies = reduce_tp(down_terms, down_land, ds, dr, n_tp)
    pending += copies
    output[...] = (resid[...].astype(jnp.float32) + down).astype(jnp.bfloat16)
    state_store.wait()
    for copy in pending:
        copy.wait_send()


def local(
    n_kv, n_tp, inner, features,
    tokens, seq_pos, state, norm_in_gain, query_weight, key_weight, value_weight, gate_weight,
    head_gain, out_weight, norm_mlp_gain, hidden_weight, down_weight,
):
    outer = n_kv // inner
    f32, bf16 = jnp.float32, jnp.bfloat16
    half = DK // 2
    inverse = jnp.power(10000.0, -jnp.arange(half, dtype=f32) / half)
    angles = seq_pos.astype(f32)[:, None] * inverse[None, :]
    cos, sin = jnp.cos(angles), jnp.sin(angles)
    cosine = jnp.concatenate([cos, cos], axis=1)
    sine = jnp.concatenate([-sin, sin], axis=1)

    own = seq_pos.shape[0]
    piece, cols = tokens.shape
    heads = state.shape[1]
    whole = heads * 2 * (DK + DV)
    hidden = hidden_weight.shape[1]
    wide = min(512, hidden // CHUNKS)
    vmem, hbm = pl.BlockSpec(memory_space=VMEM), pl.BlockSpec(memory_space=pltpu.HBM)

    def scatter_buffers(width, *lead):
        return [
            VMEM(lead + (outer, inner, own, width), bf16),
            VMEM(lead + (inner, outer, own, width), bf16),
            VMEM(lead + (outer, own, width), bf16),
            VMEM(lead + (outer, own, width), bf16),
        ]

    def two_in(*lead):
        return [DMA(lead + (inner, outer))] * 2

    def two_out(*lead):
        return [DMA(lead + (outer,))] * 2

    over_tp = [DMA((n_tp,)), DMA((n_tp,))]
    over_kv = [DMA((n_kv,)), DMA((n_kv,))]
    squares = [VMEM((n_kv, own, 128), f32), VMEM((n_kv, own, 128), f32)]
    tp_rows = VMEM((n_tp, piece, cols), bf16)
    return pl.pallas_call(
        functools.partial(layer_kernel, n_kv, n_tp, inner, features, wide),
        out_shape=[
            jax.ShapeDtypeStruct(tokens.shape, bf16),
            jax.ShapeDtypeStruct(state.shape, f32),
        ],
        in_specs=[vmem] * 2 + [hbm] * 12,
        out_specs=[vmem, hbm],
        scratch_shapes=[
            VMEM(tokens.shape, bf16), VMEM((1, cols), f32), VMEM((1, cols), f32),
            VMEM((1, heads * DV), f32),
            tp_rows, VMEM((cols, whole), bf16),
        ]
        + scatter_buffers(whole - heads * DV)
        + scatter_buffers(heads * DV)
        + squares
        + [
            VMEM((own, 2 * heads, DK), f32),
            VMEM((own, heads, DV), f32),
            VMEM((own, heads * DV), f32),
            VMEM(state.shape, f32),
            VMEM(state.shape, f32),
            VMEM((own, DK, 2 * heads), f32),
            VMEM((outer, inner, own, heads * DV), bf16),
            VMEM(out_weight.shape, bf16),
            VMEM(hidden_weight.shape, bf16),
            VMEM(down_weight.shape, bf16),
            tp_rows, tp_rows, VMEM((piece, cols), bf16), tp_rows,
        ]
        + squares
        + scatter_buffers(hidden // CHUNKS, CHUNKS)
        + [
            VMEM((CHUNKS, outer, inner, own, hidden // CHUNKS), bf16),
            VMEM((n_tp * piece, cols), f32),
            tp_rows, tp_rows,
            DMA((4,)), DMA((7,)), DMA((2,)),
        ]
        + over_tp + over_kv + two_in() + two_out() + two_in() + two_out()
        + two_out() + two_in()
        + over_tp + over_tp + over_kv
        + two_in(CHUNKS) + two_out(CHUNKS)
        + two_out(CHUNKS) + two_in(CHUNKS)
        + over_tp,
        compiler_params=pltpu.CompilerParams(
            collective_id=0, has_side_effects=True, vmem_limit_bytes=67043328
        ),
    )(
        cosine, sine, tokens, norm_in_gain[None, :], norm_mlp_gain[None, :], head_gain[None, :],
        query_weight, key_weight, value_weight, gate_weight,
        out_weight, hidden_weight, down_weight, state,
    )


def inner_size(mesh):
    column = mesh.devices[:, 0] if mesh.axis_names[0] == "kv" else mesh.devices[0, :]
    heights = [getattr(device, "coords", (0, 0, at))[2] for at, device in enumerate(column)]
    count = 1
    while count < len(heights) and heights[count] == heights[0]:
        count += 1
    return count if len(heights) % count == 0 else 1


def solution(mesh):
    n_kv, n_tp = mesh.shape["kv"], mesh.shape["tp"]
    inner = inner_size(mesh)
    placed = (
        P("tp", "kv"), P("kv"), P("kv", "tp", None, None), P("kv"),
        P("kv", "tp"), P("kv", "tp"), P("kv", "tp"), P("kv", "tp"),
        P("tp"), P("tp", "kv"), P("kv"), P("kv", "tp"), P("tp", "kv"),
    )

    def step(*args):
        return local(n_kv, n_tp, inner, args[0].shape[1] * n_kv, *args)

    return jax.shard_map(
        step, mesh=mesh, in_specs=placed,
        out_specs=(P("tp", "kv"), P("kv", "tp", None, None)), check_vma=False,
    )
```
